32 devices in a mesh: ep: 8 (over z, x), tp: 4 (over y, core).
Axes of the slice: x: 2, y: 2, z: 4, core: 2. Of those that a mesh axis runs over, the one named last changes fastest.
Arguments:
- query_latent: bfloat16 [1024, 512], P('ep'), may hold values from -6 to 6
- key_latent: bfloat16 [1024, 256], P('ep'), may hold values from -6 to 6
- rope_key: bfloat16 [1024, 64], P('ep'), may hold values from -500 to 500
- query_gain: float32 [512], replicated, may hold values from 0.1 to 1.9
- key_gain: float32 [256], replicated, may hold values from 0.1 to 1.9
- w_query: bfloat16 [512, 1024], P(None, 'tp'), may hold values from -0.25 to 0.25
- w_query_rope: bfloat16 [512, 512], P(None, 'tp'), may hold values from -0.25 to 0.25
- w_key: bfloat16 [256, 1024], P(None, 'tp'), may hold values from -0.375 to 0.375
- w_value: bfloat16 [256, 1024], P(None, 'tp'), may hold values from -0.375 to 0.375
- w_out: bfloat16 [1024, 2048], P('tp'), may hold values from -1.796875 to 1.796875
- tokens_b: bfloat16 [4096, 2048], P('ep'), may hold values from -6 to 6
- ffn_gain: float32 [2048], replicated, may hold values from 0.1 to 1.9
- route_expert: int32 [4096, 2], P('ep'), may hold values from 0 to 7, as said below
- route_weight: float32 [4096, 2], P('ep'), may hold values from 0.2 to 1
- w_gate: bfloat16 [8, 2048, 1024], P('ep', None, 'tp'), may hold values from -0.125 to 0.125
- w_up: bfloat16 [8, 2048, 1024], P('ep', None, 'tp'), may hold values from -0.125 to 0.125
- w_down: bfloat16 [8, 1024, 2048], P('ep', 'tp'), may hold values from -0.1875 to 0.1875
Outputs:
- mixer_out: bfloat16 [1024, 2048], P(('ep', 'tp'))
- moe_out: bfloat16 [4096, 2048], P('ep', 'tp')
The draws below stay inside these ranges and needn't reach their ends.
Inputs may be any that keep to these rules, and one draw needn't show every extreme that they name: `route_expert`: expert e belongs to group e // 2. A row's 2 experts differ and lie in one group. Among the rows of one device along ep, every group is named by exactly 128 rows and every expert is named exactly 128 times.
All inputs are finite; a program needn't handle non-finite values.
Results may differ from the reference program's by a relative error of at most 0.013.
The reference program's roundings to bfloat16 on the way count: a program that leaves them out, or rounds other values in their place, can miss the bound.
Values may be sent and summed in bfloat16 or wider, within the bound.
A program may use at most 64 MiB of HBM per device.

```python
import math
import jax
import jax.numpy as jnp
from jax import lax

D = 2048
HEADS = 8
NOPE = 128
ROPE = 64
VDIM = 128
QRANK = 512
KVRANK = 256
GRID_W = 64
FF_E = 1024
GROUPS = 4
TOPK = 2
TOK_A = 128
TOK_B = 512
EXPERTS = 8
TOKENS_A = 1024
TOKENS_B = 4096
N_EP = 8
N_TP = 4


def draw_rope_key(key, part):
    seq_len = TOK_A * N_EP
    key_base = jax.random.fold_in(key, 0)
    return jnp.clip(3.0 * jax.random.normal(key_base, (seq_len, ROPE), jnp.float32), -18.0, 18.0).astype(jnp.bfloat16)


def draw_route_expert(key, part):
    group_rows = TOK_B // GROUPS
    in_group = EXPERTS // GROUPS
    key_order, key_rotation, key_shift = jax.random.split(key, 3)
    ranking = jax.random.randint(key_order, (N_EP, TOK_B), 0, 1 << 16) * TOK_B + jnp.arange(TOK_B, dtype=jnp.int32)[None, :]
    ordering = jnp.argsort(ranking, axis=1, stable=True)
    position = jnp.argsort(ordering, axis=1, stable=True).astype(jnp.int32)
    group_of = position // group_rows
    within = position % group_rows
    rotation = jax.random.randint(key_rotation, (N_EP, GROUPS), 0, in_group)
    shifted = jax.random.randint(key_shift, (N_EP, GROUPS), 1, in_group)
    rotation_row = jnp.take_along_axis(rotation, group_of, axis=1)
    shift_row = jnp.take_along_axis(shifted, group_of, axis=1)
    first_choice = group_of * in_group + (within + rotation_row) % in_group
    second_choice = group_of * in_group + (within + rotation_row + shift_row) % in_group
    routes = jnp.stack([first_choice, second_choice], axis=-1)
    return routes.reshape(N_EP * TOK_B, TOPK).astype(jnp.int32)


def levels(key, extent, pieces, smallest, top_value):
    loudness = 1.0
    for dim, shards_of in pieces:
        draws = jax.random.uniform(jax.random.fold_in(jax.random.fold_in(key, 6), dim), (shards_of,), jnp.float32, smallest / len(pieces), top_value / len(pieces))
        loudness = loudness * jnp.repeat(jnp.exp(draws), extent[dim] // shards_of).reshape((-1,) + (1,) * (len(extent) - 1 - dim))
    return loudness


def noise(stream_key, shape, deviation, most, cuts=(), held_as=jnp.bfloat16):
    values = jax.random.normal(stream_key, shape, jnp.float32) * deviation
    if len(cuts) > 0:
        values = levels(stream_key, shape, cuts, -0.22, 0.18) * values
    return jnp.clip(values, min=-most, max=most).astype(held_as)


def setup_inputs(seed: int = 0) -> dict:
    key_of = jax.random.split(jax.random.key(seed), 18)
    query_latent = noise(key_of[0], (TOKENS_A, QRANK), 1.0, 6.0, ((0, 8),))
    key_latent = noise(key_of[1], (TOKENS_A, KVRANK), 1.0, 6.0, ((0, 8),))
    rope_key = draw_rope_key(jax.random.fold_in(key_of[17], 71), 0)
    query_gain = jnp.clip(1.0 + 0.18 * jax.random.normal(key_of[3], (QRANK,), jnp.float32), 0.1, 1.9)
    key_gain = jnp.clip(1.0 + 0.18 * jax.random.normal(key_of[4], (KVRANK,), jnp.float32), 0.1, 1.9)
    w_query = noise(key_of[5], (QRANK, HEADS * NOPE), QRANK ** -0.5, 0.25, ((1, 4),))
    w_query_rope = noise(key_of[6], (QRANK, HEADS * ROPE), QRANK ** -0.5, 0.25, ((1, 4),))
    w_key = noise(key_of[7], (KVRANK, HEADS * NOPE), KVRANK ** -0.5, 0.375, ((1, 4),))
    w_value = noise(key_of[8], (KVRANK, HEADS * VDIM), KVRANK ** -0.5, 0.375, ((1, 4),))
    w_out = noise(key_of[9], (HEADS * VDIM, D), 0.3, 1.796875, ((0, 4),))
    tokens_b = noise(key_of[10], (TOKENS_B, D), 1.0, 6.0, ((0, 8),))
    ffn_gain = jnp.clip(1.0 + 0.18 * jax.random.normal(key_of[11], (D,), jnp.float32), 0.1, 1.9)
    route_expert = draw_route_expert(jax.random.fold_in(key_of[17], 71), 0)
    route_weight = jnp.clip(jnp.exp(math.log(1.0) - 1.609438 * jax.random.uniform(key_of[13], (TOKENS_B, TOPK), jnp.float32) ** levels(key_of[13], (TOKENS_B, TOPK), ((0, 8),), -0.2, 0.2)), 0.2, 1.0)
    w_gate = noise(key_of[14], (EXPERTS, D, FF_E), D ** -0.5, 0.125, ((0, 8), (2, 4)))
    w_up = noise(key_of[15], (EXPERTS, D, FF_E), D ** -0.5, 0.125, ((0, 8), (2, 4)))
    w_down = noise(key_of[16], (EXPERTS, FF_E, D), FF_E ** -0.5, 0.1875, ((0, 8), (1, 4)))
    return {"query_latent": query_latent, "key_latent": key_latent, "rope_key": rope_key, "query_gain": query_gain, "key_gain": key_gain, "w_query": w_query, "w_query_rope": w_query_rope, "w_key": w_key, "w_value": w_value, "w_out": w_out, "tokens_b": tokens_b, "ffn_gain": ffn_gain, "route_expert": route_expert, "route_weight": route_weight, "w_gate": w_gate, "w_up": w_up, "w_down": w_down}


epsilon = 1e-06
rotary_base = 10000.0

def rms_scale(values_in, gain):
    widened = values_in.astype(jnp.float32)
    normed = widened * lax.rsqrt(lax.optimization_barrier(jnp.mean(widened * widened, axis=-1, keepdims=True)) + epsilon)
    return (normed * gain.astype(jnp.float32)).astype(jnp.bfloat16)

def rotary_tables(positions):
    half_width = ROPE // 2
    inverse = rotary_base ** (-jnp.arange(0, half_width, 2, dtype=jnp.float32) / half_width)
    grid_row = (positions // GRID_W).astype(jnp.float32)
    grid_col = (positions % GRID_W).astype(jnp.float32)
    angle = jnp.concatenate([grid_row[:, None] * inverse, grid_col[:, None] * inverse], axis=-1)
    return (jnp.cos(angle), jnp.sin(angle))

def rotate(values_in, cosine, sine):
    even_part = values_in[..., 0::2]
    odd_part = values_in[..., 1::2]
    turned = jnp.stack([even_part * cosine - odd_part * sine, even_part * sine + odd_part * cosine], axis=-1)
    return turned.reshape(values_in.shape)

def mixer_half(query_latent, key_latent, rope_key, query_gain, key_gain, w_query, w_query_rope, w_key, w_value, w_out):
    seq_len = query_latent.shape[0]
    positions = jnp.arange(seq_len, dtype=jnp.int32)
    cosine, sine = rotary_tables(positions)
    query_normed = rms_scale(query_latent, query_gain)
    query_nope = jnp.dot(query_normed, w_query, preferred_element_type=jnp.float32).astype(jnp.bfloat16)
    query_nope = query_nope.reshape(seq_len, HEADS, NOPE)
    query_rot = jnp.dot(query_normed, w_query_rope, preferred_element_type=jnp.float32).reshape(seq_len, HEADS, ROPE)
    query_rot = rotate(query_rot, cosine[:, None, :], sine[:, None, :]).astype(jnp.bfloat16)
    key_normed = rms_scale(key_latent, key_gain)
    key_nope = jnp.dot(key_normed, w_key, preferred_element_type=jnp.float32).astype(jnp.bfloat16)
    key_nope = key_nope.reshape(seq_len, HEADS, NOPE)
    value_rows = jnp.dot(key_normed, w_value, preferred_element_type=jnp.float32).astype(jnp.bfloat16)
    value_rows = value_rows.reshape(seq_len, HEADS, VDIM)
    key_rot = rotate(rope_key.astype(jnp.float32), cosine, sine).astype(jnp.bfloat16)
    score_scale = (NOPE + ROPE) ** (-0.5)
    block_rows = math.gcd(seq_len, 512)

    def one_head(operands):
        head_query, head_rot, head_key, head_value = operands

        def one_block(block_operands):
            block_query, block_rot = block_operands
            scores = jnp.dot(block_query, head_key.T, preferred_element_type=jnp.float32)
            scores = (scores + jnp.dot(block_rot, key_rot.T, preferred_element_type=jnp.float32)) * score_scale
            row_max = lax.optimization_barrier(jnp.max(scores, axis=-1, keepdims=True))
            weights = jnp.exp(scores - row_max)
            totals = lax.optimization_barrier(jnp.sum(weights, axis=-1, keepdims=True))
            mixed = jnp.dot(weights.astype(jnp.bfloat16), head_value, preferred_element_type=jnp.float32)
            return (mixed / totals).astype(jnp.bfloat16)
        blocks = lax.map(one_block, (head_query.reshape(seq_len // block_rows, block_rows, NOPE), head_rot.reshape(seq_len // block_rows, block_rows, ROPE)))
        return blocks.reshape(seq_len, VDIM)
    heads_out = lax.map(one_head, (jnp.moveaxis(query_nope, 1, 0), jnp.moveaxis(query_rot, 1, 0), jnp.moveaxis(key_nope, 1, 0), jnp.moveaxis(value_rows, 1, 0)))
    heads_flat = jnp.moveaxis(heads_out, 0, 1).reshape(seq_len, HEADS * VDIM)
    group_cols = HEADS * VDIM // N_TP
    summed = jnp.zeros((seq_len, D), jnp.float32)
    for group_index in range(N_TP):
        lower = group_index * group_cols
        piece_sum = jnp.dot(heads_flat[:, lower:lower + group_cols], w_out[lower:lower + group_cols], preferred_element_type=jnp.float32).astype(jnp.bfloat16)
        summed = summed + lax.optimization_barrier(piece_sum).astype(jnp.float32)
    return summed.astype(jnp.bfloat16)

def expert_half(tokens_b, ffn_gain, route_expert, route_weight, w_gate, w_up, w_down):
    all_rows = tokens_b.shape[0]
    capacity = TOPK * TOK_B // EXPERTS
    normed = rms_scale(tokens_b, ffn_gain)
    copies = route_expert.reshape(N_EP, TOK_B * TOPK)
    expert_ids = jnp.arange(EXPERTS, dtype=jnp.int32)

    def block_slots(block_copies):
        chosen = (block_copies[:, None] == expert_ids[None, :]).astype(jnp.int32)
        earlier = jnp.cumsum(chosen, axis=0) - chosen
        return lax.optimization_barrier(jnp.sum(earlier * chosen, axis=1)).astype(jnp.int32)
    slot_index = lax.map(block_slots, copies)
    block_ids = jnp.arange(N_EP, dtype=jnp.int32)[:, None]
    target = (copies * (N_EP * capacity) + block_ids * capacity + slot_index).reshape(-1).astype(jnp.int32)
    source_row = jnp.zeros((EXPERTS * N_EP * capacity,), jnp.int32).at[target].set(jnp.arange(all_rows * TOPK, dtype=jnp.int32) // TOPK)
    source_row = source_row.reshape(EXPERTS, N_EP * capacity)
    unit_cols = FF_E // N_TP

    def one_expert(operands):
        row_ids, gate_weight, up_weight, down_weight = operands
        arrived = jnp.take(normed, row_ids, axis=0)
        gate_act = jnp.dot(arrived, gate_weight, preferred_element_type=jnp.float32)
        up_act = jnp.dot(arrived, up_weight, preferred_element_type=jnp.float32)
        hidden = (jax.nn.silu(gate_act) * up_act).astype(jnp.bfloat16)
        summed = jnp.zeros((arrived.shape[0], D), jnp.float32)
        for group_index in range(N_TP):
            lower = group_index * unit_cols
            piece_sum = jnp.dot(hidden[:, lower:lower + unit_cols], down_weight[lower:lower + unit_cols], preferred_element_type=jnp.float32).astype(jnp.bfloat16)
            summed = summed + lax.optimization_barrier(piece_sum).astype(jnp.float32)
        return summed.astype(jnp.bfloat16)
    results = lax.map(one_expert, (source_row, w_gate, w_up, w_down)).reshape(EXPERTS * N_EP * capacity, D)
    picked = jnp.take(results, target, axis=0).reshape(all_rows, TOPK, D)
    combined = lax.optimization_barrier(jnp.sum(picked.astype(jnp.float32) * route_weight[:, :, None], axis=1))
    return combined.astype(jnp.bfloat16)

def reference(query_latent, key_latent, rope_key, query_gain, key_gain, w_query, w_query_rope, w_key, w_value, w_out, tokens_b, ffn_gain, route_expert, route_weight, w_gate, w_up, w_down):
    mixer_out = mixer_half(query_latent, key_latent, rope_key, query_gain, key_gain, w_query, w_query_rope, w_key, w_value, w_out)
    moe_out = expert_half(tokens_b, ffn_gain, route_expert, route_weight, w_gate, w_up, w_down)
    return (mixer_out, moe_out)
```

```python
import math

import jax
import jax.numpy as jnp
from jax import lax
from jax.experimental import pallas as pl
from jax.experimental.pallas import tpu as pltpu
from jax.sharding import PartitionSpec as P

NOPE = 128
ROPE = 64
VDIM = 128
GRID_W = 64
TOPK = 2
GROUPS = 4
MESH = pl.DeviceIdType.MESH
SPLIT_NUM, SPLIT_DEN = 3, 8
JOIN_FIRST = (1, 3)


epsilon = 1e-06
rotary_base = 10000.0
neg_large = -1e30


def rms_scale(values_in, gain):
    widened = values_in.astype(jnp.float32)
    normed = widened * lax.rsqrt(jnp.mean(widened * widened, axis=-1, keepdims=True) + epsilon)
    return (normed * gain).astype(jnp.bfloat16)


def rotary_tables(positions):
    half_width = ROPE // 2
    inverse = rotary_base ** (-jnp.arange(0, half_width, 2, dtype=jnp.float32) / half_width)
    grid_row = (positions // GRID_W).astype(jnp.float32)
    grid_col = (positions % GRID_W).astype(jnp.float32)
    angle = jnp.concatenate([grid_row[:, None] * inverse, grid_col[:, None] * inverse], axis=-1)
    return (jnp.cos(angle), jnp.sin(angle))


def rotate(values_in, cosine, sine):
    even_part = values_in[..., 0::2]
    odd_part = values_in[..., 1::2]
    turned = jnp.stack(
        [even_part * cosine - odd_part * sine, even_part * sine + odd_part * cosine], axis=-1
    )
    return turned.reshape(values_in.shape)


def fold_blocks(carry, members, step_fn):
    piece_rows = members[0].shape[0]
    block_rows = math.gcd(piece_rows, 1024)
    if block_rows == piece_rows:
        return step_fn(carry, members)
    stacked = tuple(
        (
            member.reshape((piece_rows // block_rows, block_rows) + member.shape[1:])
            for member in members
        )
    )

    def scan_step(inner_carry, blocks):
        return (step_fn(inner_carry, blocks), None)

    result, unused = lax.scan(scan_step, carry, stacked)
    return result


def mixer_half(
    query_latent,
    key_latent,
    rope_key,
    query_gain,
    key_gain,
    w_query,
    w_query_rope,
    w_key,
    w_value,
    w_out,
):
    tok_rows = query_latent.shape[0]
    local_heads = w_query.shape[1] // NOPE
    positions = lax.axis_index("ep") * tok_rows + jnp.arange(tok_rows, dtype=jnp.int32)
    cosine, sine = rotary_tables(positions)
    query_normed = rms_scale(query_latent, query_gain)
    query_nope = jnp.dot(query_normed, w_query, preferred_element_type=jnp.float32).astype(
        jnp.bfloat16
    )
    query_nope = query_nope.reshape(tok_rows, local_heads, NOPE)
    query_rot = jnp.dot(query_normed, w_query_rope, preferred_element_type=jnp.float32)
    query_rot = rotate(
        query_rot.reshape(tok_rows, local_heads, ROPE), cosine[:, None, :], sine[:, None, :]
    )
    query_rot = query_rot.astype(jnp.bfloat16)
    key_rot = rotate(rope_key.astype(jnp.float32), cosine, sine).astype(jnp.bfloat16)
    score_scale = (NOPE + ROPE) ** (-0.5)

    def expand(latent_rows):
        latent_count = latent_rows.shape[0]
        key_normed = rms_scale(latent_rows, key_gain)
        key_nope = jnp.dot(key_normed, w_key, preferred_element_type=jnp.float32).astype(
            jnp.bfloat16
        )
        value_rows = jnp.dot(key_normed, w_value, preferred_element_type=jnp.float32).astype(
            jnp.bfloat16
        )
        return (
            key_nope.reshape(latent_count, local_heads, NOPE),
            value_rows.reshape(latent_count, local_heads, VDIM),
        )

    def attend_block(carry, key_nope, value_rows, key_turn):
        run_max, run_total, run_acc = carry
        scores = jnp.einsum(
            "qhd,khd->hqk", query_nope, key_nope, preferred_element_type=jnp.float32
        )
        scores = scores + jnp.einsum(
            "qhd,kd->hqk", query_rot, key_turn, preferred_element_type=jnp.float32
        )
        scores = scores * score_scale
        new_max = jnp.maximum(run_max, jnp.max(scores, axis=-1))
        correction = jnp.exp(run_max - new_max)
        weights = jnp.exp(scores - new_max[..., None])
        new_total = run_total * correction + jnp.sum(weights, axis=-1)
        added = jnp.einsum(
            "hqk,khd->qhd",
            weights.astype(jnp.bfloat16),
            value_rows,
            preferred_element_type=jnp.float32,
        )
        new_acc = run_acc * jnp.transpose(correction)[..., None] + added
        return (new_max, new_total, new_acc)

    def step_latent(carry, blocks):
        key_nope, value_rows = expand(blocks[0])
        return attend_block(carry, key_nope, value_rows, blocks[1])

    initial = (
        jnp.full((local_heads, tok_rows), neg_large, jnp.float32),
        jnp.zeros((local_heads, tok_rows), jnp.float32),
        jnp.zeros((tok_rows, local_heads, VDIM), jnp.float32),
    )
    gathered = lax.all_gather(
        jnp.concatenate([key_latent, key_rot], axis=1), "ep", axis=0, tiled=True
    )
    rank = key_latent.shape[1]
    final = fold_blocks(initial, (gathered[:, :rank], gathered[:, rank:]), step_latent)
    run_max, run_total, run_acc = final
    heads_out = (run_acc / jnp.transpose(run_total)[..., None]).astype(jnp.bfloat16)
    heads_out = heads_out.reshape(tok_rows, local_heads * VDIM)
    return lax.psum_scatter(
        jnp.dot(heads_out, w_out, preferred_element_type=jnp.float32).astype(jnp.bfloat16),
        "tp",
        scatter_dimension=0,
        tiled=True,
    )


def expert_half(tokens_b, ffn_gain, route_expert, route_weight, w_gate, w_up, w_down):
    tok_rows = tokens_b.shape[0]
    expert_count = lax.axis_size("ep")
    capacity = TOPK * tok_rows // expert_count
    normed = rms_scale(tokens_b, ffn_gain)
    copies = route_expert.reshape(tok_rows * TOPK)
    chosen = (copies[:, None] == jnp.arange(expert_count, dtype=jnp.int32)[None, :]).astype(
        jnp.int32
    )
    earlier = jnp.cumsum(chosen, axis=0) - chosen
    slot_index = jnp.sum(earlier * chosen, axis=1)
    target = copies * capacity + slot_index
    source_row = (
        jnp.zeros((expert_count * capacity,), jnp.int32)
        .at[target]
        .set(jnp.arange(tok_rows * TOPK, dtype=jnp.int32) // TOPK)
    )
    outgoing = jnp.take(normed, source_row, axis=0)
    share_cols = outgoing.shape[1] // lax.axis_size("tp")
    own_cols = lax.dynamic_slice_in_dim(outgoing, lax.axis_index("tp") * share_cols, share_cols, 1)
    arrived = lax.all_to_all(own_cols, "ep", split_axis=0, concat_axis=0, tiled=True)
    member = lax.all_gather(arrived, "tp", axis=1, tiled=True)
    gate_rows = w_gate[0]
    up_rows = w_up[0]
    gate_act = jnp.dot(member, gate_rows, preferred_element_type=jnp.float32)
    up_act = jnp.dot(member, up_rows, preferred_element_type=jnp.float32)
    hidden = (jax.nn.silu(gate_act) * up_act).astype(jnp.bfloat16)
    partial_term = jnp.dot(hidden, w_down[0], preferred_element_type=jnp.float32)
    shared = lax.psum_scatter(
        partial_term.astype(jnp.bfloat16), "tp", scatter_dimension=1, tiled=True
    )
    returned = lax.all_to_all(shared, "ep", split_axis=0, concat_axis=0, tiled=True)
    picked = (
        jnp.take(returned, target, axis=0)
        .astype(jnp.float32)
        .reshape(tok_rows, TOPK, returned.shape[1])
    )
    combined = jnp.sum(picked * route_weight[:, :, None], axis=1)
    return combined.astype(jnp.bfloat16)


def flip(index, distance):
    low = index % 2
    high = index // 2
    if distance % 2 == 1:
        low = 1 - low
    if distance // 2 == 1:
        high = 1 - high
    return high * 2 + low


def expert_kernel(
    tokens_ref,
    gain_ref,
    order_ref,
    weight_ref,
    gate_hbm,
    up_hbm,
    down_hbm,
    fin_ref,
    normed_ref,
    outgoing_ref,
    member_ref,
    gate_ref,
    up_ref,
    down_ref,
    weight_in,
    pair_send,
    pair_keep,
    pair_recv,
    first_send,
    first_keep,
    first_recv,
    second_send,
    second_keep,
    second_recv,
    fin_send,
    load_sem,
    z_send,
    z_recv,
    w_send,
    w_recv,
    x_send,
    x_recv,
    y_send,
    y_recv,
    c_send,
    c_recv,
    p_send,
    p_recv,
    f_send,
    f_recv,
    s_send,
    s_recv,
    o_send,
    o_recv,
):
    ep = lax.axis_index("ep")
    tp = lax.axis_index("tp")
    z, x = ep // 2, ep % 2
    y, c = tp // 2, tp % 2
    rows = outgoing_ref.shape[2]
    half = outgoing_ref.shape[3]
    tok_rows = tokens_ref.shape[0]
    share = fin_ref.shape[2]
    spare = rows * SPLIT_NUM // SPLIT_DEN
    carried = pl.ds(pl.multiple_of(y * spare, 16), rows - spare)
    passed = pl.ds(pl.multiple_of(y * (rows - spare), 16), spare)

    def at_z(distance):
        return {"ep": flip(z, distance) * 2 + x, "tp": tp}

    at_x = {"ep": z * 2 + 1 - x, "tp": tp}
    at_y = {"ep": ep, "tp": (1 - y) * 2 + c}
    at_c = {"ep": ep, "tp": y * 2 + 1 - c}

    barrier = pltpu.get_barrier_semaphore()
    for peer in (at_z(1), at_z(2), at_z(3), at_x, at_y, at_c):
        pl.semaphore_signal(barrier, inc=1, device_id=peer, device_id_type=MESH)

    loads = [
        pltpu.make_async_copy(gate_hbm.at[0], gate_ref, load_sem.at[0]),
        pltpu.make_async_copy(up_hbm.at[0], up_ref, load_sem.at[1]),
    ]
    for t in range(4):
        loads.append(
            pltpu.make_async_copy(
                down_hbm.at[0, :, pl.ds(t * share, share)], down_ref.at[t], load_sem.at[2 + t]
            )
        )
    for load in loads:
        load.start()

    step_rows = 32

    def norm_step(step, unused):
        lines = pl.ds(pl.multiple_of(step * step_rows, step_rows), step_rows)
        widened = tokens_ref[lines, :].astype(jnp.float32)
        mean = jnp.mean(widened * widened, axis=-1, keepdims=True)
        normed = widened * lax.rsqrt(mean + epsilon) * gain_ref[...]
        normed_ref[lines, :] = normed.astype(jnp.bfloat16)
        return unused

    lax.fori_loop(0, tok_rows // step_rows, norm_step, 0)

    def permuted(group, part):
        lines = pl.ds(pl.multiple_of(group * rows, rows), rows)
        return jnp.dot(
            order_ref[lines, :],
            normed_ref[:, part * half : (part + 1) * half],
            preferred_element_type=jnp.float32,
        ).astype(jnp.bfloat16)

    def remote(source, target, send, recv, peer):
        return pltpu.make_async_remote_copy(
            src_ref=source,
            dst_ref=target,
            send_sem=send,
            recv_sem=recv,
            device_id=peer,
            device_id_type=MESH,
        )

    def z_copy(d):
        return remote(
            outgoing_ref.at[flip(z, d), c, carried],
            member_ref.at[c, z, x, carried],
            z_send.at[d],
            z_recv.at[d],
            at_z(d),
        )

    def w_copy(d):
        return remote(
            weight_ref.at[flip(z, d)], weight_in.at[z], w_send.at[d], w_recv.at[d], at_z(d)
        )

    def x_copy(d):
        block = member_ref.at[c, flip(z, d), x, carried]
        return remote(block, block, x_send.at[d], x_recv.at[d], at_x)

    def y_copy(k):
        line = x if k % 2 == 0 else 1 - x
        block = member_ref.at[c, flip(z, k // 2), line, passed]
        return remote(block, block, y_send.at[k], y_recv.at[k], at_y)

    def c_copy(k):
        line = x if k % 2 == 0 else 1 - x
        block = member_ref.at[c, flip(z, k // 2), line]
        return remote(block, block, c_send.at[k], c_recv.at[k], at_c)

    def p_copy(d):
        return remote(pair_send.at[d], pair_recv.at[d], p_send.at[d], p_recv.at[d], at_c)

    def f_copy(d):
        peer = at_x if d in JOIN_FIRST else at_y
        return remote(first_send.at[d], first_recv.at[d], f_send.at[d], f_recv.at[d], peer)

    def s_copy(d):
        peer = at_y if d in JOIN_FIRST else at_x
        return remote(second_send.at[d], second_recv.at[d], s_send.at[d], s_recv.at[d], peer)

    def o_copy(d):
        return remote(fin_send.at[d], fin_ref.at[z], o_send.at[d], o_recv.at[d], at_z(d))

    started = []

    def start(copy):
        copy.start()
        started.append(copy)

    for part in range(2):
        member_ref[part, z, x] = permuted(z, part)
    pl.semaphore_wait(barrier, 6)
    start(x_copy(0))
    for d in (1, 3, 2):
        for part in range(2):
            outgoing_ref[flip(z, d), part] = permuted(flip(z, d), part)
        start(z_copy(d))
        start(w_copy(d))

    def compute(d):
        block = flip(z, d)
        low = member_ref[0, block].reshape(2 * rows, half)
        high = member_ref[1, block].reshape(2 * rows, half)

        def project(weights):
            return jnp.dot(
                low, weights[:half, :], preferred_element_type=jnp.float32
            ) + jnp.dot(high, weights[half:, :], preferred_element_type=jnp.float32)

        gate_act = project(gate_ref)
        up_act = project(up_ref)
        hidden = (gate_act / (1.0 + jnp.exp(-gate_act)) * up_act).astype(jnp.bfloat16)
        for yy in range(2):
            term = jnp.dot(hidden, down_ref[yy * 2 + 1 - c], preferred_element_type=jnp.float32)
            pair_send[d, yy] = term.astype(jnp.bfloat16).reshape(2, rows, share)
        start(p_copy(d))
        for yy in range(2):
            term = jnp.dot(hidden, down_ref[yy * 2 + c], preferred_element_type=jnp.float32)
            pair_keep[d, yy] = term.astype(jnp.bfloat16).reshape(2, rows, share)

    def weights_of(d):
        tile = weight_ref[z] if d == 0 else weight_in[flip(z, d)]
        mine = jnp.where(x == 0, tile[0:1], tile[1:2])
        other = jnp.where(x == 0, tile[1:2], tile[0:1])

        def columns(line):
            square = jnp.transpose(jnp.broadcast_to(line, (rows, rows)))
            return jnp.concatenate([square] * (share // rows), axis=1)

        return columns(mine), columns(other)

    def wide(value):
        return value.astype(jnp.float32)

    def stage_first(d):
        p_copy(d).wait_recv()
        if d in JOIN_FIRST:
            for yy in range(2):
                sums = wide(pair_keep[d, yy, 1 - x]) + wide(pair_recv[d, yy, 1 - x])
                first_send[d, yy] = sums.astype(jnp.bfloat16)
            start(f_copy(d))
            for yy in range(2):
                first_keep[d, yy] = wide(pair_keep[d, yy, x]) + wide(pair_recv[d, yy, x])
        else:
            for line in range(2):
                sums = wide(pair_keep[d, 1 - y, line]) + wide(pair_recv[d, 1 - y, line])
                first_send[d, line] = sums.astype(jnp.bfloat16)
            start(f_copy(d))
            for line in range(2):
                first_keep[d, line] = wide(pair_keep[d, y, line]) + wide(pair_recv[d, y, line])

    def stage_second(d):
        f_copy(d).wait_recv()
        if d in JOIN_FIRST:
            if d > 0:
                w_copy(d).wait_recv()
            mine, other = weights_of(d)
            sums = mine * first_keep[d, 1 - y] + other * wide(first_recv[d, 1 - y])
            second_send[d] = sums.astype(jnp.bfloat16)
            start(s_copy(d))
            second_keep[d] = mine * first_keep[d, y] + other * wide(first_recv[d, y])
        else:
            sums = first_keep[d, 1 - x] + wide(first_recv[d, 1 - x])
            second_send[d] = sums.astype(jnp.bfloat16)
            start(s_copy(d))
            sums = first_keep[d, x] + wide(first_recv[d, x])
            second_keep[d] = wide(sums.astype(jnp.bfloat16))

    def stage_last(d):
        s_copy(d).wait_recv()
        if d in JOIN_FIRST:
            result = second_keep[d] + wide(second_recv[d])
        else:
            if d > 0:
                w_copy(d).wait_recv()
            mine, other = weights_of(d)
            result = mine * second_keep[d] + other * wide(second_recv[d])
        if d == 0:
            fin_ref[z] = result.astype(jnp.bfloat16)
        else:
            fin_send[d] = result.astype(jnp.bfloat16)
            start(o_copy(d))

    def from_z(d):
        z_copy(d).wait_recv()
        start(x_copy(d))
        start(y_copy(2 * d))

    def from_x(d):
        x_copy(d).wait_recv()
        start(y_copy(2 * d + 1))

    def from_y(k):
        y_copy(k).wait_recv()
        start(c_copy(k))

    from_z(1)
    from_x(0)
    for load in loads:
        load.wait()
    from_y(2)
    from_y(1)
    from_x(1)
    c_copy(1).wait_recv()
    compute(0)
    from_y(3)
    stage_first(0)
    c_copy(2).wait_recv()
    c_copy(3).wait_recv()
    compute(1)
    from_z(3)
    stage_first(1)
    stage_second(0)
    from_z(2)
    from_x(3)
    from_y(6)
    from_x(2)
    from_y(4)
    from_y(7)
    stage_second(1)
    stage_last(0)
    c_copy(6).wait_recv()
    c_copy(7).wait_recv()
    compute(3)
    from_y(5)
    stage_first(3)
    c_copy(4).wait_recv()
    c_copy(5).wait_recv()
    compute(2)
    stage_last(1)
    stage_first(2)
    stage_second(3)
    stage_second(2)
    stage_last(3)
    stage_last(2)
    for d in (1, 3, 2):
        o_copy(d).wait_recv()
    for copy in started:
        copy.wait_send()


def expert_exchange(tokens_b, ffn_gain, order, weights, w_gate, w_up, w_down):
    tok_rows, width = tokens_b.shape
    rows = tok_rows // GROUPS
    half = width // 2
    share = width // 4
    units = w_gate.shape[2]
    narrow, full = jnp.bfloat16, jnp.float32
    vmem = pl.BlockSpec(memory_space=pltpu.VMEM)
    anywhere = pl.BlockSpec(memory_space=pl.ANY)
    dma = pltpu.SemaphoreType.DMA
    return pl.pallas_call(
        expert_kernel,
        out_shape=jax.ShapeDtypeStruct((GROUPS, rows, share), narrow),
        in_specs=[vmem] * 4 + [anywhere] * 3,
        out_specs=vmem,
        scratch_shapes=[
            pltpu.VMEM((tok_rows, width), narrow),
            pltpu.VMEM((GROUPS, 2, rows, half), narrow),
            pltpu.VMEM((2, GROUPS, 2, rows, half), narrow),
            pltpu.VMEM((width, units), narrow),
            pltpu.VMEM((width, units), narrow),
            pltpu.VMEM((4, units, share), narrow),
            pltpu.VMEM(weights.shape, full),
            pltpu.VMEM((GROUPS, 2, 2, rows, share), narrow),
            pltpu.VMEM((GROUPS, 2, 2, rows, share), narrow),
            pltpu.VMEM((GROUPS, 2, 2, rows, share), narrow),
            pltpu.VMEM((GROUPS, 2, rows, share), narrow),
            pltpu.VMEM((GROUPS, 2, rows, share), full),
            pltpu.VMEM((GROUPS, 2, rows, share), narrow),
            pltpu.VMEM((GROUPS, rows, share), narrow),
            pltpu.VMEM((GROUPS, rows, share), full),
            pltpu.VMEM((GROUPS, rows, share), narrow),
            pltpu.VMEM((GROUPS, rows, share), narrow),
            dma((6,)),
        ]
        + [dma((4,))] * 6
        + [dma((8,))] * 4
        + [dma((4,))] * 8,
        compiler_params=pltpu.CompilerParams(
            collective_id=0, has_side_effects=True, vmem_limit_bytes=52 * 1024 * 1024
        ),
        cost_estimate=pl.CostEstimate(
            flops=40_000_000_000, bytes_accessed=8_000_000, transcendentals=0
        ),
        name="expert_exchange",
    )(tokens_b, ffn_gain.reshape(1, width), order, weights, w_gate, w_up, w_down)


def expert_half_paired(tokens_b, ffn_gain, route_expert, route_weight, w_gate, w_up, w_down):
    tok_rows = tokens_b.shape[0]
    group = route_expert[:, 0] // TOPK
    chosen = (group[:, None] == jnp.arange(GROUPS, dtype=jnp.int32)[None, :]).astype(jnp.bfloat16)
    line = jnp.arange(tok_rows, dtype=jnp.int32)
    before = (line[None, :] < line[:, None]).astype(jnp.bfloat16)
    earlier = jnp.dot(before, chosen, preferred_element_type=jnp.float32)
    rank = jnp.sum(earlier * chosen.astype(jnp.float32), axis=1).astype(jnp.int32)
    place = group * (tok_rows // GROUPS) + rank
    hit = line[:, None] == place[None, :]
    order = hit.astype(jnp.bfloat16)
    first_even = route_expert[:, 0] % TOPK == 0
    even = jnp.where(first_even, route_weight[:, 0], route_weight[:, 1])
    odd = jnp.where(first_even, route_weight[:, 1], route_weight[:, 0])
    sorted_even = jnp.sum(jnp.where(hit, even[None, :], 0.0), axis=1)
    sorted_odd = jnp.sum(jnp.where(hit, odd[None, :], 0.0), axis=1)
    rows = tok_rows // GROUPS
    weights = jnp.stack([sorted_even.reshape(GROUPS, rows), sorted_odd.reshape(GROUPS, rows)], axis=1)
    weights = jnp.pad(weights, ((0, 0), (0, 8 - TOPK), (0, 0)))
    fin = expert_exchange(tokens_b, ffn_gain, order, weights, w_gate, w_up, w_down)
    fin = fin.reshape(tok_rows, fin.shape[2])
    back = lax.dot_general(order, fin, (((0,), (0,)), ((), ())), preferred_element_type=jnp.float32)
    return back.astype(jnp.bfloat16)


def body(
    query_latent,
    key_latent,
    rope_key,
    query_gain,
    key_gain,
    w_query,
    w_query_rope,
    w_key,
    w_value,
    w_out,
    tokens_b,
    ffn_gain,
    route_expert,
    route_weight,
    w_gate,
    w_up,
    w_down,
):
    mixer_out = mixer_half(
        query_latent,
        key_latent,
        rope_key,
        query_gain,
        key_gain,
        w_query,
        w_query_rope,
        w_key,
        w_value,
        w_out,
    )
    paired = (
        lax.axis_size("ep") == GROUPS * TOPK
        and lax.axis_size("tp") == 4
        and GROUPS == 4
        and tokens_b.shape[0] == GROUPS * 128
    )
    experts = expert_half_paired if paired else expert_half
    moe_out = experts(tokens_b, ffn_gain, route_expert, route_weight, w_gate, w_up, w_down)
    return (mixer_out, moe_out)


def solution(mesh):
    in_specs = (
        P("ep", None),
        P("ep", None),
        P("ep", None),
        P(),
        P(),
        P(None, "tp"),
        P(None, "tp"),
        P(None, "tp"),
        P(None, "tp"),
        P("tp", None),
        P("ep", None),
        P(),
        P("ep", None),
        P("ep", None),
        P("ep", None, "tp"),
        P("ep", None, "tp"),
        P("ep", "tp", None),
    )
    out_specs = (P(("ep", "tp"), None), P("ep", "tp"))
    return jax.shard_map(body, mesh=mesh, in_specs=in_specs, out_specs=out_specs, check_vma=False)
```

```python
import math

import jax
import jax.numpy as jnp
from jax import lax
from jax.experimental import pallas as pl
from jax.experimental.pallas import tpu as pltpu
from jax.sharding import PartitionSpec as P

NOPE = 128
ROPE = 64
VDIM = 128
GRID_W = 64
TOPK = 2
GROUPS = 4
MESH = pl.DeviceIdType.MESH
SPLIT_NUM, SPLIT_DEN = 1, 8
JOIN_FIRST = ()


epsilon = 1e-06
rotary_base = 10000.0
neg_large = -1e30


def rms_scale(values_in, gain):
    widened = values_in.astype(jnp.float32)
    normed = widened * lax.rsqrt(jnp.mean(widened * widened, axis=-1, keepdims=True) + epsilon)
    return (normed * gain).astype(jnp.bfloat16)


def rotary_tables(positions):
    half_width = ROPE // 2
    inverse = rotary_base ** (-jnp.arange(0, half_width, 2, dtype=jnp.float32) / half_width)
    grid_row = (positions // GRID_W).astype(jnp.float32)
    grid_col = (positions % GRID_W).astype(jnp.float32)
    angle = jnp.concatenate([grid_row[:, None] * inverse, grid_col[:, None] * inverse], axis=-1)
    return (jnp.cos(angle), jnp.sin(angle))


def rotate(values_in, cosine, sine):
    even_part = values_in[..., 0::2]
    odd_part = values_in[..., 1::2]
    turned = jnp.stack(
        [even_part * cosine - odd_part * sine, even_part * sine + odd_part * cosine], axis=-1
    )
    return turned.reshape(values_in.shape)


def fold_blocks(carry, members, step_fn):
    piece_rows = members[0].shape[0]
    block_rows = math.gcd(piece_rows, 1024)
    if block_rows == piece_rows:
        return step_fn(carry, members)
    stacked = tuple(
        (
            member.reshape((piece_rows // block_rows, block_rows) + member.shape[1:])
            for member in members
        )
    )

    def scan_step(inner_carry, blocks):
        return (step_fn(inner_carry, blocks), None)

    result, unused = lax.scan(scan_step, carry, stacked)
    return result


def mixer_half(
    query_latent,
    key_latent,
    rope_key,
    query_gain,
    key_gain,
    w_query,
    w_query_rope,
    w_key,
    w_value,
    w_out,
):
    tok_rows = query_latent.shape[0]
    local_heads = w_query.shape[1] // NOPE
    positions = lax.axis_index("ep") * tok_rows + jnp.arange(tok_rows, dtype=jnp.int32)
    cosine, sine = rotary_tables(positions)
    query_normed = rms_scale(query_latent, query_gain)
    query_nope = jnp.dot(query_normed, w_query, preferred_element_type=jnp.float32).astype(
        jnp.bfloat16
    )
    query_nope = query_nope.reshape(tok_rows, local_heads, NOPE)
    query_rot = jnp.dot(query_normed, w_query_rope, preferred_element_type=jnp.float32)
    query_rot = rotate(
        query_rot.reshape(tok_rows, local_heads, ROPE), cosine[:, None, :], sine[:, None, :]
    )
    query_rot = query_rot.astype(jnp.bfloat16)
    key_rot = rotate(rope_key.astype(jnp.float32), cosine, sine).astype(jnp.bfloat16)
    score_scale = (NOPE + ROPE) ** (-0.5)

    def expand(latent_rows):
        latent_count = latent_rows.shape[0]
        key_normed = rms_scale(latent_rows, key_gain)
        key_nope = jnp.dot(key_normed, w_key, preferred_element_type=jnp.float32).astype(
            jnp.bfloat16
        )
        value_rows = jnp.dot(key_normed, w_value, preferred_element_type=jnp.float32).astype(
            jnp.bfloat16
        )
        return (
            key_nope.reshape(latent_count, local_heads, NOPE),
            value_rows.reshape(latent_count, local_heads, VDIM),
        )

    def attend_block(carry, key_nope, value_rows, key_turn):
        run_max, run_total, run_acc = carry
        scores = jnp.einsum(
            "qhd,khd->hqk", query_nope, key_nope, preferred_element_type=jnp.float32
        )
        scores = scores + jnp.einsum(
            "qhd,kd->hqk", query_rot, key_turn, preferred_element_type=jnp.float32
        )
        scores = scores * score_scale
        new_max = jnp.maximum(run_max, jnp.max(scores, axis=-1))
        correction = jnp.exp(run_max - new_max)
        weights = jnp.exp(scores - new_max[..., None])
        new_total = run_total * correction + jnp.sum(weights, axis=-1)
        added = jnp.einsum(
            "hqk,khd->qhd",
            weights.astype(jnp.bfloat16),
            value_rows,
            preferred_element_type=jnp.float32,
        )
        new_acc = run_acc * jnp.transpose(correction)[..., None] + added
        return (new_max, new_total, new_acc)

    def step_latent(carry, blocks):
        key_nope, value_rows = expand(blocks[0])
        return attend_block(carry, key_nope, value_rows, blocks[1])

    initial = (
        jnp.full((local_heads, tok_rows), neg_large, jnp.float32),
        jnp.zeros((local_heads, tok_rows), jnp.float32),
        jnp.zeros((tok_rows, local_heads, VDIM), jnp.float32),
    )
    gathered = lax.all_gather(
        jnp.concatenate([key_latent, key_rot], axis=1), "ep", axis=0, tiled=True
    )
    rank = key_latent.shape[1]
    final = fold_blocks(initial, (gathered[:, :rank], gathered[:, rank:]), step_latent)
    run_max, run_total, run_acc = final
    heads_out = (run_acc / jnp.transpose(run_total)[..., None]).astype(jnp.bfloat16)
    heads_out = heads_out.reshape(tok_rows, local_heads * VDIM)
    return lax.psum_scatter(
        jnp.dot(heads_out, w_out, preferred_element_type=jnp.float32).astype(jnp.bfloat16),
        "tp",
        scatter_dimension=0,
        tiled=True,
    )


def expert_half(tokens_b, ffn_gain, route_expert, route_weight, w_gate, w_up, w_down):
    tok_rows = tokens_b.shape[0]
    expert_count = lax.axis_size("ep")
    capacity = TOPK * tok_rows // expert_count
    normed = rms_scale(tokens_b, ffn_gain)
    copies = route_expert.reshape(tok_rows * TOPK)
    chosen = (copies[:, None] == jnp.arange(expert_count, dtype=jnp.int32)[None, :]).astype(
        jnp.int32
    )
    earlier = jnp.cumsum(chosen, axis=0) - chosen
    slot_index = jnp.sum(earlier * chosen, axis=1)
    target = copies * capacity + slot_index
    source_row = (
        jnp.zeros((expert_count * capacity,), jnp.int32)
        .at[target]
        .set(jnp.arange(tok_rows * TOPK, dtype=jnp.int32) // TOPK)
    )
    outgoing = jnp.take(normed, source_row, axis=0)
    share_cols = outgoing.shape[1] // lax.axis_size("tp")
    own_cols = lax.dynamic_slice_in_dim(outgoing, lax.axis_index("tp") * share_cols, share_cols, 1)
    arrived = lax.all_to_all(own_cols, "ep", split_axis=0, concat_axis=0, tiled=True)
    member = lax.all_gather(arrived, "tp", axis=1, tiled=True)
    gate_rows = w_gate[0]
    up_rows = w_up[0]
    gate_act = jnp.dot(member, gate_rows, preferred_element_type=jnp.float32)
    up_act = jnp.dot(member, up_rows, preferred_element_type=jnp.float32)
    hidden = (jax.nn.silu(gate_act) * up_act).astype(jnp.bfloat16)
    partial_term = jnp.dot(hidden, w_down[0], preferred_element_type=jnp.float32)
    shared = lax.psum_scatter(
        partial_term.astype(jnp.bfloat16), "tp", scatter_dimension=1, tiled=True
    )
    returned = lax.all_to_all(shared, "ep", split_axis=0, concat_axis=0, tiled=True)
    picked = (
        jnp.take(returned, target, axis=0)
        .astype(jnp.float32)
        .reshape(tok_rows, TOPK, returned.shape[1])
    )
    combined = jnp.sum(picked * route_weight[:, :, None], axis=1)
    return combined.astype(jnp.bfloat16)


def flip(index, distance):
    low = index % 2
    high = index // 2
    if distance % 2 == 1:
        low = 1 - low
    if distance // 2 == 1:
        high = 1 - high
    return high * 2 + low


def expert_kernel(
    tokens_ref,
    gain_ref,
    order_ref,
    weight_ref,
    gate_hbm,
    up_hbm,
    down_hbm,
    query_ref,
    latent_ref,
    rope_ref,
    query_gain_ref,
    key_gain_ref,
    cosine_ref,
    sine_ref,
    w_query_ref,
    w_rope_ref,
    w_key_ref,
    w_value_ref,
    w_out_ref,
    fin_ref,
    mixer_ref,
    normed_ref,
    outgoing_ref,
    member_ref,
    gate_ref,
    up_ref,
    down_ref,
    weight_in,
    pair_send,
    pair_keep,
    pair_recv,
    first_send,
    first_keep,
    first_recv,
    second_send,
    second_keep,
    second_recv,
    fin_send,
    keys_ref,
    heads_ref,
    mixed_ref,
    mixed_in,
    joint_send,
    joint_recv,
    load_sem,
    z_send,
    z_recv,
    w_send,
    w_recv,
    x_send,
    x_recv,
    y_send,
    y_recv,
    c_send,
    c_recv,
    p_send,
    p_recv,
    f_send,
    f_recv,
    s_send,
    s_recv,
    o_send,
    o_recv,
    kz_send,
    kz_recv,
    kx_send,
    kx_recv,
    kc_send,
    kc_recv,
    a_send,
    a_recv,
    j_send,
    j_recv,
):
    ep = lax.axis_index("ep")
    tp = lax.axis_index("tp")
    z, x = ep // 2, ep % 2
    y, c = tp // 2, tp % 2
    rows = outgoing_ref.shape[2]
    half = outgoing_ref.shape[3]
    tok_rows = tokens_ref.shape[0]
    share = fin_ref.shape[2]
    spare = rows * SPLIT_NUM // SPLIT_DEN
    carried = pl.ds(pl.multiple_of(y * spare, 16), rows - spare)
    passed = pl.ds(pl.multiple_of(y * (rows - spare), 16), spare)

    def at_z(distance):
        return {"ep": flip(z, distance) * 2 + x, "tp": tp}

    at_x = {"ep": z * 2 + 1 - x, "tp": tp}
    at_y = {"ep": ep, "tp": (1 - y) * 2 + c}
    at_c = {"ep": ep, "tp": y * 2 + 1 - c}

    barrier = pltpu.get_barrier_semaphore()
    for peer in (at_z(1), at_z(2), at_z(3), at_x, at_y, at_c):
        pl.semaphore_signal(barrier, inc=1, device_id=peer, device_id_type=MESH)

    loads = [
        pltpu.make_async_copy(gate_hbm.at[0], gate_ref, load_sem.at[0]),
        pltpu.make_async_copy(up_hbm.at[0], up_ref, load_sem.at[1]),
    ]
    for t in range(4):
        loads.append(
            pltpu.make_async_copy(
                down_hbm.at[0, :, pl.ds(t * share, share)], down_ref.at[t], load_sem.at[2 + t]
            )
        )
    for load in loads:
        load.start()

    def scaled(values_in, gain):
        widened = values_in.astype(jnp.float32)
        mean = jnp.mean(widened * widened, axis=-1, keepdims=True)
        return (widened * lax.rsqrt(mean + epsilon) * gain).astype(jnp.bfloat16)

    turn_shape = (w_rope_ref.shape[1], w_rope_ref.shape[1])
    from_lane = lax.broadcasted_iota(jnp.int32, turn_shape, 0)
    to_lane = lax.broadcasted_iota(jnp.int32, turn_shape, 1)
    to_even = to_lane % 2 == 0
    swap = jnp.where(to_even & (from_lane == to_lane + 1), -1.0, 0.0)
    swap = jnp.where(jnp.logical_not(to_even) & (from_lane == to_lane - 1), 1.0, swap)
    swap = swap.astype(jnp.bfloat16)

    def dot(left, right):
        return jnp.dot(left, right, preferred_element_type=jnp.float32)

    attend_rows, rank = latent_ref.shape
    rope_twice = jnp.concatenate([rope_ref[...]] * 2, axis=1)
    key_turn = rope_twice.astype(jnp.float32) * cosine_ref[...]
    key_turn = key_turn + dot(rope_twice, swap) * sine_ref[...]
    keys_ref[z, x, :, :rank] = scaled(latent_ref[...], key_gain_ref[...])
    keys_ref[z, x, :, rank:] = key_turn.astype(jnp.bfloat16)

    step_rows = 32

    def norm_step(step, unused):
        lines = pl.ds(pl.multiple_of(step * step_rows, step_rows), step_rows)
        normed_ref[lines, :] = scaled(tokens_ref[lines, :], gain_ref[...])
        return unused

    def permuted(group, part):
        lines = pl.ds(pl.multiple_of(group * rows, rows), rows)
        return jnp.dot(
            order_ref[lines, :],
            normed_ref[:, part * half : (part + 1) * half],
            preferred_element_type=jnp.float32,
        ).astype(jnp.bfloat16)

    def remote(source, target, send, recv, peer):
        return pltpu.make_async_remote_copy(
            src_ref=source,
            dst_ref=target,
            send_sem=send,
            recv_sem=recv,
            device_id=peer,
            device_id_type=MESH,
        )

    def z_copy(d):
        return remote(
            outgoing_ref.at[flip(z, d), c, carried],
            member_ref.at[c, z, x, carried],
            z_send.at[d],
            z_recv.at[d],
            at_z(d),
        )

    def w_copy(d):
        return remote(
            weight_ref.at[flip(z, d)], weight_in.at[z], w_send.at[d], w_recv.at[d], at_z(d)
        )

    def x_copy(d):
        block = member_ref.at[c, flip(z, d), x, carried]
        return remote(block, block, x_send.at[d], x_recv.at[d], at_x)

    def y_copy(k):
        line = x if k % 2 == 0 else 1 - x
        block = member_ref.at[c, flip(z, k // 2), line, passed]
        return remote(block, block, y_send.at[k], y_recv.at[k], at_y)

    def c_copy(k):
        line = x if k % 2 == 0 else 1 - x
        block = member_ref.at[c, flip(z, k // 2), line]
        return remote(block, block, c_send.at[k], c_recv.at[k], at_c)

    def p_copy(d):
        return remote(pair_send.at[d], pair_recv.at[d], p_send.at[d], p_recv.at[d], at_c)

    def f_copy(d):
        peer = at_x if d in JOIN_FIRST else at_y
        return remote(first_send.at[d], first_recv.at[d], f_send.at[d], f_recv.at[d], peer)

    def s_copy(d):
        peer = at_y if d in JOIN_FIRST else at_x
        return remote(second_send.at[d], second_recv.at[d], s_send.at[d], s_recv.at[d], peer)

    def o_copy(d):
        return remote(fin_send.at[d], fin_ref.at[z], o_send.at[d], o_recv.at[d], at_z(d))

    key_half = pl.ds(pl.multiple_of(c * (attend_rows // 2), 16), attend_rows // 2)

    def kz_copy(d):
        block = keys_ref.at[z, x, key_half]
        return remote(block, block, kz_send.at[d], kz_recv.at[d], at_z(d))

    def kx_copy(d):
        block = keys_ref.at[flip(z, d), x, key_half]
        return remote(block, block, kx_send.at[d], kx_recv.at[d], at_x)

    def kc_copy(d):
        if d == 0:
            block = keys_ref.at[z, 1 - x, key_half]
        else:
            block = keys_ref.at[flip(z, d), :, key_half]
        return remote(block, block, kc_send.at[d], kc_recv.at[d], at_c)

    def a_copy(yy):
        return remote(
            mixed_ref.at[yy * 2 + 1 - c], mixed_in.at[yy], a_send.at[yy], a_recv.at[yy], at_c
        )

    def j_copy():
        return remote(joint_send, joint_recv, j_send.at[0], j_recv.at[0], at_y)

    started = []

    def start(copy):
        copy.start()
        started.append(copy)

    pl.semaphore_wait(barrier, 6)
    start(kx_copy(0))
    for d in (1, 3, 2):
        start(kz_copy(d))
    lax.fori_loop(0, tok_rows // step_rows, norm_step, 0)
    for part in range(2):
        member_ref[part, z, x] = permuted(z, part)
    start(x_copy(0))
    for d in (1, 3, 2):
        for part in range(2):
            outgoing_ref[flip(z, d), part] = permuted(flip(z, d), part)
        start(z_copy(d))
        start(w_copy(d))

    def compute(d):
        block = flip(z, d)
        low = member_ref[0, block].reshape(2 * rows, half)
        high = member_ref[1, block].reshape(2 * rows, half)

        def project(weights):
            return jnp.dot(
                low, weights[:half, :], preferred_element_type=jnp.float32
            ) + jnp.dot(high, weights[half:, :], preferred_element_type=jnp.float32)

        gate_act = project(gate_ref)
        up_act = project(up_ref)
        hidden = (gate_act / (1.0 + jnp.exp(-gate_act)) * up_act).astype(jnp.bfloat16)
        for yy in range(2):
            term = jnp.dot(hidden, down_ref[yy * 2 + 1 - c], preferred_element_type=jnp.float32)
            pair_send[d, yy] = term.astype(jnp.bfloat16).reshape(2, rows, share)
        start(p_copy(d))
        for yy in range(2):
            term = jnp.dot(hidden, down_ref[yy * 2 + c], preferred_element_type=jnp.float32)
            pair_keep[d, yy] = term.astype(jnp.bfloat16).reshape(2, rows, share)

    def weights_of(d):
        tile = weight_ref[z] if d == 0 else weight_in[flip(z, d)]
        mine = jnp.where(x == 0, tile[0:1], tile[1:2])
        other = jnp.where(x == 0, tile[1:2], tile[0:1])

        def columns(line):
            square = jnp.transpose(jnp.broadcast_to(line, (rows, rows)))
            return jnp.concatenate([square] * (share // rows), axis=1)

        return columns(mine), columns(other)

    def attend():
        query_normed = scaled(query_ref[...], query_gain_ref[...])
        query_nope = dot(query_normed, w_query_ref[...]).astype(jnp.bfloat16)
        swapped = dot(w_rope_ref[...], swap).astype(jnp.bfloat16)
        query_turn = dot(query_normed, w_rope_ref[...]) * cosine_ref[...]
        query_turn = query_turn + dot(query_normed, swapped) * sine_ref[...]
        query_turn = query_turn.astype(jnp.bfloat16)
        count = keys_ref.shape[0] * keys_ref.shape[1] * attend_rows
        keys = keys_ref[...].reshape(count, keys_ref.shape[3])
        latents, turned = keys[:, :rank], keys[:, rank:]
        key_nope = dot(latents, w_key_ref[...]).astype(jnp.bfloat16)
        value_rows = dot(latents, w_value_ref[...]).astype(jnp.bfloat16)
        lane = lax.broadcasted_iota(jnp.int32, query_turn.shape, 1)
        for head in range(w_query_ref.shape[1] // NOPE):
            own = slice(head * NOPE, (head + 1) * NOPE)
            part = jnp.where(lane // ROPE == head, query_turn, jnp.zeros_like(query_turn))
            scores = lax.dot_general(
                jnp.concatenate([query_nope[:, own], part], axis=1),
                jnp.concatenate([key_nope[:, own], turned], axis=1),
                (((1,), (1,)), ((), ())),
                preferred_element_type=jnp.float32,
            )
            scores = scores * (NOPE + ROPE) ** (-0.5)
            raised = jnp.exp(scores - jnp.max(scores, axis=-1, keepdims=True))
            totals = jnp.sum(raised, axis=-1, keepdims=True)
            mixed = dot(raised.astype(jnp.bfloat16), value_rows[:, own]) / totals
            heads_ref[:, own] = mixed.astype(jnp.bfloat16)
        for t in range(4):
            lines = slice(t * (attend_rows // 4), (t + 1) * (attend_rows // 4))
            mixed_ref[t] = dot(heads_ref[lines, :], w_out_ref[...]).astype(jnp.bfloat16)
        for yy in range(2):
            start(a_copy(yy))

    def attend_join():
        for yy in range(2):
            a_copy(yy).wait_recv()
        sums = wide(mixed_ref[(1 - y) * 2 + c]) + wide(mixed_in[1 - y])
        joint_send[...] = sums.astype(jnp.bfloat16)
        start(j_copy())

    def attend_last():
        j_copy().wait_recv()
        sums = wide(mixed_ref[y * 2 + c]) + wide(mixed_in[y]) + wide(joint_recv[...])
        mixer_ref[...] = sums.astype(jnp.bfloat16)

    def wide(value):
        return value.astype(jnp.float32)

    def stage_first(d):
        p_copy(d).wait_recv()
        if d in JOIN_FIRST:
            for yy in range(2):
                sums = wide(pair_keep[d, yy, 1 - x]) + wide(pair_recv[d, yy, 1 - x])
                first_send[d, yy] = sums.astype(jnp.bfloat16)
            start(f_copy(d))
            for yy in range(2):
                first_keep[d, yy] = wide(pair_keep[d, yy, x]) + wide(pair_recv[d, yy, x])
        else:
            for line in range(2):
                sums = wide(pair_keep[d, 1 - y, line]) + wide(pair_recv[d, 1 - y, line])
                first_send[d, line] = sums.astype(jnp.bfloat16)
            start(f_copy(d))
            for line in range(2):
                first_keep[d, line] = wide(pair_keep[d, y, line]) + wide(pair_recv[d, y, line])

    def stage_second(d):
        f_copy(d).wait_recv()
        if d in JOIN_FIRST:
            if d > 0:
                w_copy(d).wait_recv()
            mine, other = weights_of(d)
            sums = mine * first_keep[d, 1 - y] + other * wide(first_recv[d, 1 - y])
            second_send[d] = sums.astype(jnp.bfloat16)
            start(s_copy(d))
            second_keep[d] = mine * first_keep[d, y] + other * wide(first_recv[d, y])
        else:
            sums = first_keep[d, 1 - x] + wide(first_recv[d, 1 - x])
            second_send[d] = sums.astype(jnp.bfloat16)
            start(s_copy(d))
            sums = first_keep[d, x] + wide(first_recv[d, x])
            second_keep[d] = wide(sums.astype(jnp.bfloat16))

    def stage_last(d):
        s_copy(d).wait_recv()
        if d in JOIN_FIRST:
            result = second_keep[d] + wide(second_recv[d])
        else:
            if d > 0:
                w_copy(d).wait_recv()
            mine, other = weights_of(d)
            result = mine * second_keep[d] + other * wide(second_recv[d])
        if d == 0:
            fin_ref[z] = result.astype(jnp.bfloat16)
        else:
            fin_send[d] = result.astype(jnp.bfloat16)
            start(o_copy(d))

    def from_z(d):
        z_copy(d).wait_recv()
        start(x_copy(d))
        start(y_copy(2 * d))

    def from_x(d):
        x_copy(d).wait_recv()
        start(y_copy(2 * d + 1))

    def from_y(k):
        y_copy(k).wait_recv()
        start(c_copy(k))

    for d in (1, 3, 2):
        kz_copy(d).wait_recv()
        start(kx_copy(d))
    for d in (0, 1, 3, 2):
        kx_copy(d).wait_recv()
        start(kc_copy(d))
    from_z(1)
    from_x(0)
    for load in loads:
        load.wait()
    from_y(2)
    from_y(1)
    from_x(1)
    c_copy(1).wait_recv()
    compute(0)
    from_y(3)
    stage_first(0)
    c_copy(2).wait_recv()
    c_copy(3).wait_recv()
    from_z(3)
    compute(1)
    for d in range(4):
        kc_copy(d).wait_recv()
    attend()
    stage_first(1)
    stage_second(0)
    from_z(2)
    from_x(3)
    from_y(6)
    from_x(2)
    from_y(4)
    from_y(7)
    stage_second(1)
    stage_last(0)
    c_copy(6).wait_recv()
    c_copy(7).wait_recv()
    compute(3)
    from_y(5)
    stage_first(3)
    attend_join()
    c_copy(4).wait_recv()
    c_copy(5).wait_recv()
    compute(2)
    stage_last(1)
    stage_first(2)
    stage_second(3)
    attend_last()
    stage_second(2)
    stage_last(3)
    stage_last(2)
    for d in (1, 3, 2):
        o_copy(d).wait_recv()
    for copy in started:
        copy.wait_send()


def expert_exchange(tokens_b, ffn_gain, order, weights, w_gate, w_up, w_down, mixer_args):
    tok_rows, width = tokens_b.shape
    rows = tok_rows // GROUPS
    half = width // 2
    share = width // 4
    units = w_gate.shape[2]
    attend_rows, rank = mixer_args[1].shape
    key_cols = rank + 2 * ROPE
    head_cols = mixer_args[7].shape[1]
    narrow, full = jnp.bfloat16, jnp.float32
    vmem = pl.BlockSpec(memory_space=pltpu.VMEM)
    anywhere = pl.BlockSpec(memory_space=pl.ANY)
    dma = pltpu.SemaphoreType.DMA
    return pl.pallas_call(
        expert_kernel,
        out_shape=(
            jax.ShapeDtypeStruct((GROUPS, rows, share), narrow),
            jax.ShapeDtypeStruct((attend_rows // 4, width), narrow),
        ),
        in_specs=[vmem] * 4 + [anywhere] * 3 + [vmem] * 12,
        out_specs=(vmem, vmem),
        scratch_shapes=[
            pltpu.VMEM((tok_rows, width), narrow),
            pltpu.VMEM((GROUPS, 2, rows, half), narrow),
            pltpu.VMEM((2, GROUPS, 2, rows, half), narrow),
            pltpu.VMEM((width, units), narrow),
            pltpu.VMEM((width, units), narrow),
            pltpu.VMEM((4, units, share), narrow),
            pltpu.VMEM(weights.shape, full),
            pltpu.VMEM((GROUPS, 2, 2, rows, share), narrow),
            pltpu.VMEM((GROUPS, 2, 2, rows, share), narrow),
            pltpu.VMEM((GROUPS, 2, 2, rows, share), narrow),
            pltpu.VMEM((GROUPS, 2, rows, share), narrow),
            pltpu.VMEM((GROUPS, 2, rows, share), full),
            pltpu.VMEM((GROUPS, 2, rows, share), narrow),
            pltpu.VMEM((GROUPS, rows, share), narrow),
            pltpu.VMEM((GROUPS, rows, share), full),
            pltpu.VMEM((GROUPS, rows, share), narrow),
            pltpu.VMEM((GROUPS, rows, share), narrow),
            pltpu.VMEM((GROUPS, 2, attend_rows, key_cols), narrow),
            pltpu.VMEM((attend_rows, head_cols), narrow),
            pltpu.VMEM((4, attend_rows // 4, width), narrow),
            pltpu.VMEM((2, attend_rows // 4, width), narrow),
            pltpu.VMEM((attend_rows // 4, width), narrow),
            pltpu.VMEM((attend_rows // 4, width), narrow),
            dma((6,)),
        ]
        + [dma((4,))] * 6
        + [dma((8,))] * 4
        + [dma((4,))] * 14
        + [dma((2,))] * 4,
        compiler_params=pltpu.CompilerParams(
            collective_id=0, has_side_effects=True, vmem_limit_bytes=52 * 1024 * 1024
        ),
        cost_estimate=pl.CostEstimate(
            flops=40_000_000_000, bytes_accessed=8_000_000, transcendentals=0
        ),
        name="expert_exchange",
    )(tokens_b, ffn_gain.reshape(1, width), order, weights, w_gate, w_up, w_down, *mixer_args)


def lane_tables(tok_rows, width):
    positions = lax.axis_index("ep") * tok_rows + lax.broadcasted_iota(
        jnp.int32, (tok_rows, width), 0
    )
    pair = lax.broadcasted_iota(jnp.int32, (tok_rows, width), 1) % ROPE // 2
    half_width = ROPE // 2
    quarter = half_width // 2
    inverse = rotary_base ** (-(pair % quarter * 2).astype(jnp.float32) / half_width)
    grid_row = (positions // GRID_W).astype(jnp.float32)
    grid_col = (positions % GRID_W).astype(jnp.float32)
    angle = jnp.where(pair < quarter, grid_row, grid_col) * inverse
    return (jnp.cos(angle), jnp.sin(angle))


def paired(mixer, tokens_b, ffn_gain, route_expert, route_weight, w_gate, w_up, w_down):
    tok_rows = tokens_b.shape[0]
    group = route_expert[:, 0] // TOPK
    chosen = (group[:, None] == jnp.arange(GROUPS, dtype=jnp.int32)[None, :]).astype(jnp.bfloat16)
    line = jnp.arange(tok_rows, dtype=jnp.int32)
    before = (line[None, :] < line[:, None]).astype(jnp.bfloat16)
    earlier = jnp.dot(before, chosen, preferred_element_type=jnp.float32)
    rank = jnp.sum(earlier * chosen.astype(jnp.float32), axis=1).astype(jnp.int32)
    place = group * (tok_rows // GROUPS) + rank
    hit = line[:, None] == place[None, :]
    order = hit.astype(jnp.bfloat16)
    first_even = route_expert[:, 0] % TOPK == 0
    even = jnp.where(first_even, route_weight[:, 0], route_weight[:, 1])
    odd = jnp.where(first_even, route_weight[:, 1], route_weight[:, 0])
    sorted_even = jnp.sum(jnp.where(hit, even[None, :], 0.0), axis=1)
    sorted_odd = jnp.sum(jnp.where(hit, odd[None, :], 0.0), axis=1)
    rows = tok_rows // GROUPS
    weights = jnp.stack([sorted_even.reshape(GROUPS, rows), sorted_odd.reshape(GROUPS, rows)], axis=1)
    weights = jnp.pad(weights, ((0, 0), (0, 8 - TOPK), (0, 0)))
    query_latent, key_latent, rope_key, query_gain, key_gain = mixer[:5]
    mixer_args = (
        query_latent,
        key_latent,
        rope_key,
        query_gain.reshape(1, -1),
        key_gain.reshape(1, -1),
        *lane_tables(query_latent.shape[0], 2 * ROPE),
        *mixer[5:],
    )
    fin, mixer_out = expert_exchange(
        tokens_b, ffn_gain, order, weights, w_gate, w_up, w_down, mixer_args
    )
    fin = fin.reshape(tok_rows, fin.shape[2])
    back = lax.dot_general(order, fin, (((0,), (0,)), ((), ())), preferred_element_type=jnp.float32)
    return (mixer_out, back.astype(jnp.bfloat16))


def body(
    query_latent,
    key_latent,
    rope_key,
    query_gain,
    key_gain,
    w_query,
    w_query_rope,
    w_key,
    w_value,
    w_out,
    tokens_b,
    ffn_gain,
    route_expert,
    route_weight,
    w_gate,
    w_up,
    w_down,
):
    mixer = (
        query_latent,
        key_latent,
        rope_key,
        query_gain,
        key_gain,
        w_query,
        w_query_rope,
        w_key,
        w_value,
        w_out,
    )
    experts = (tokens_b, ffn_gain, route_expert, route_weight, w_gate, w_up, w_down)
    if (
        lax.axis_size("ep") == GROUPS * TOPK
        and lax.axis_size("tp") == 4
        and GROUPS == 4
        and tokens_b.shape[0] == GROUPS * 128
        and w_query.shape[1] == 2 * NOPE
    ):
        return paired(mixer, *experts)
    return (mixer_half(*mixer), expert_half(*experts))


def solution(mesh):
    in_specs = (
        P("ep", None),
        P("ep", None),
        P("ep", None),
        P(),
        P(),
        P(None, "tp"),
        P(None, "tp"),
        P(None, "tp"),
        P(None, "tp"),
        P("tp", None),
        P("ep", None),
        P(),
        P("ep", None),
        P("ep", None),
        P("ep", None, "tp"),
        P("ep", None, "tp"),
        P("ep", "tp", None),
    )
    out_specs = (P(("ep", "tp"), None), P("ep", "tp"))
    return jax.shard_map(body, mesh=mesh, in_specs=in_specs, out_specs=out_specs, check_vma=False)
```
